32 devices in a mesh: ep: 8 (over z, x), tp: 4 (over y, core).
Axes of the slice: x: 2, y: 2, z: 4, core: 2. Of those that a mesh axis runs over, the one named last changes fastest.
Arguments:
- mix_tokens: bfloat16 [4096, 2048], P('ep'), may hold values from -6 to 6
- mix_gain: float32 [2048], replicated, may hold values from 0.1 to 1.9
- w_query: bfloat16 [2048, 2048], P(None, 'tp'), may hold values from -0.125 to 0.125
- w_forget_fwd: bfloat16 [2048, 2048], P(None, 'tp'), may hold values from -0.125 to 0.125
- w_forget_bwd: bfloat16 [2048, 2048], P(None, 'tp'), may hold values from -0.125 to 0.125
- w_value: bfloat16 [2048, 2048], P(None, 'tp'), may hold values from -0.125 to 0.125
- decay_floor: float32 [2048], P('tp'), may hold values from 0.975 to 1
- decay_shift: float32 [4096, 16], P('ep', 'tp'), may hold values from -1.3 to 0
- head_gain: float32 [128], replicated, may hold values from 0.1 to 1.9
- w_out: bfloat16 [2048, 2048], replicated, may hold values from -0.125 to 0.125
- moe_tokens: bfloat16 [3072, 2048], P('ep'), may hold values from -6 to 6
- moe_gain: float32 [2048], replicated, may hold values from 0.1 to 1.9
- routes: int32 [3072, 2], P('ep'), may hold values from 0 to 7, all different within a row; in each aligned block of 384 rows (0 to 383, 384 to 767, ...) at most 144 rows name the same one
- route_logits: float32 [3072, 2], P('ep'), may hold values from -6 to 6
- w_expert_gate: bfloat16 [8, 2048, 5120], P('ep', None, 'tp'), may hold values from -0.125 to 0.125
- w_expert_up: bfloat16 [8, 2048, 5120], P('ep', None, 'tp'), may hold values from -0.125 to 0.125
- w_expert_down: bfloat16 [8, 5120, 2048], P('ep', 'tp'), may hold values from -0.078125 to 0.078125
Outputs:
- mixed_out: bfloat16 [4096, 2048], P(('ep', 'tp'))
- moe_out: bfloat16 [3072, 2048], P('ep', 'tp')
The draws below stay inside these ranges and needn't reach their ends.
Inputs may be any that keep to these rules, and one draw needn't show every extreme that they name: `routes`: in each aligned block of 384 rows (the rows of one index of ep) no expert is named by more than 144 rows, and in some block an expert is named by exactly 144; the two entries of a row differ.
All inputs are finite; a program needn't handle non-finite values.
Results may differ from the reference program's by a relative error of at most 0.014.
Values may be sent and summed in bfloat16 or wider, within the bound.
A program may use at most 128 MiB of HBM per device.

```python
import functools
import math
import jax
import jax.numpy as jnp
import numpy as np
from jax import lax

D = 2048
HEADS = 16
DK = 128
DV = 128
FF = 5120
TOPK = 2
M_EP = 384
SEG = 512
ROWS = 4096
MROWS = 3072
EXPERTS = 8
CAP = 144
N_EP = 8
N_TP = 4


def decay_table(key):
    head_key = jax.random.fold_in(key, 11)
    scores = jax.random.randint(jax.random.fold_in(head_key, 1), (HEADS,), 0, 1000)
    forced = jax.random.randint(jax.random.fold_in(head_key, 2), (), 0, HEADS)
    limit = 500
    return (scores < limit) | (jnp.arange(HEADS) == forced)


def draw_decay_floor(key, part):
    fast = decay_table(key)
    rate = jnp.where(fast, 1.0 / 40.0, 0.2 / ROWS).astype(jnp.float32)
    spread = jax.random.uniform(jax.random.fold_in(key, 21), (HEADS, DK), jnp.float32, 0.5, 1.0)
    return (1.0 - rate[:, None] * spread).reshape(HEADS * DK)


def draw_decay_shift(key, part):
    fast = decay_table(key)
    start_offset = jnp.where(fast, 1.0 / 40.0, 0.25 / ROWS).astype(jnp.float32)
    block_total = ROWS // SEG
    factor = jnp.exp(jax.random.uniform(jax.random.fold_in(key, 31), (block_total, HEADS), jnp.float32, math.log(0.5), math.log(2.0)))
    row_amounts = jnp.repeat(factor, SEG, axis=0)
    slot_locations = jax.random.randint(jax.random.fold_in(key, 32), (2, HEADS), 0, ROWS)
    loss_values = jax.random.uniform(jax.random.fold_in(key, 33), (2, HEADS), jnp.float32, 0.2, 0.45)
    row_identifiers = jnp.arange(ROWS)[:, None]
    token_groups = jnp.where(row_identifiers == slot_locations[0][None, :], jnp.log1p(-loss_values[0])[None, :], 0.0) + jnp.where(row_identifiers == slot_locations[1][None, :], jnp.log1p(-loss_values[1])[None, :], 0.0)
    return (-start_offset[None, :] * row_amounts + token_groups).astype(jnp.float32)


def block_levels(rng, shape, shards, low, top_value):
    def one(dim, blocks):
        heights = jax.random.uniform(jax.random.fold_in(jax.random.fold_in(rng, 6), dim), (blocks,), jnp.float32, low / len(shards), top_value / len(shards))
        return jnp.repeat(jnp.exp(heights), shape[dim] // blocks).reshape((-1,) + (1,) * (len(shape) - dim - 1))

    loudness = one(*shards[0])
    for cut in shards[1:]:
        loudness = loudness * one(*cut)
    return loudness


def shared_out(own_key, own, number, rows, number_of, top, bound, skew):
    ranking = jax.random.permutation(own_key, number_of)
    packed, common = load_shares(number_of, rows * top, bound, skew, True), load_shares(number_of, rows * top, bound, skew, False)
    places = jnp.arange(number_of)

    def named(lengths, offset_by):
        used = int((lengths > 0).sum())
        fixed = max(1, used // 4)
        passed = fixed + (places - fixed + offset_by * (used - fixed)) % max(1, number_of - fixed)
        return jnp.zeros((number_of,), jnp.int32).at[ranking[jnp.where(places < fixed, places, passed)]].set(jnp.asarray(lengths, jnp.int32))

    lengths = jnp.where(number % 4 == 0, named(packed, number // 4), named(common, number - number // 4 - 1))
    mixed = jax.random.permutation(jax.random.fold_in(own, 3), number_of)
    donor, sink = mixed[0:number_of // 2 * 2:2], mixed[1:number_of // 2 * 2:2]
    slack = jnp.minimum(lengths[donor] - 1, bound - lengths[sink]) // 2
    slack = jnp.where((donor == ranking[0]) | (sink == ranking[0]) | (lengths[sink] == 0), 0, jnp.maximum(slack, 0))
    passed = jax.random.randint(jax.random.fold_in(own, 4), (number_of // 2,), 0, 1 << 20) % (slack + 1)
    lengths = lengths.at[donor].add(-passed).at[sink].add(passed)
    labels = jnp.searchsorted(jnp.cumsum(lengths), jnp.arange(rows * top), side="right").astype(jnp.int32)
    listing = labels.reshape(top, rows).T
    listing = listing[jax.random.permutation(jax.random.fold_in(own, 1), rows)]
    offset_by = jax.random.randint(jax.random.fold_in(own, 2), (rows, 1), 0, top)
    return jnp.take_along_axis(listing, (jnp.arange(top)[None, :] + offset_by) % top, axis=1)


def load_shares(count, total, reach, lean, full):
    portions = [(1 << 20) // math.isqrt(rank ** lean) + 1 for rank in range(1, count + 1)]
    largest = reach if full else min(reach, max(-(-total // count), total * portions[0] // sum(portions)))
    least = 1 if total - largest >= count - 1 else 0
    holding, surplus = [largest] + [least] * (count - 1), total - largest - least * (count - 1)
    while surplus > 0:
        free = [i for i in range(1, count) if holding[i] < largest] or [i for i in range(1, count) if holding[i] < reach]
        whole, remaining = sum([portions[i] for i in free]), surplus
        for i in free:
            more = min(reach - holding[i], max(1, remaining * portions[i] // whole), surplus)
            holding[i] = holding[i] + more
            surplus = surplus - more
    return np.array(holding)


def gaussian(key, shape, scale, most, cuts=(), held_as=jnp.bfloat16):
    values = scale * jax.random.normal(key, shape, jnp.float32)
    if cuts:
        values = values * block_levels(key, shape, cuts, -0.22, 0.18)
    return jnp.clip(values, -most, most).astype(held_as)


def setup_inputs(seed: int = 0) -> dict:
    splits = jax.random.split(jax.random.key(seed), 18)
    mix_tokens = gaussian(splits[0], (ROWS, D), 1.0, 6.0, ((0, 8),))
    mix_gain = jnp.clip(1.0 + 0.18 * jax.random.normal(splits[1], (D,), jnp.float32), 0.1, 1.9)
    w_query = gaussian(splits[2], (D, HEADS * DK), D ** -0.5, 0.125, ((1, 4),))
    w_forget_fwd = gaussian(splits[3], (D, HEADS * DK), D ** -0.5, 0.125, ((1, 4),))
    w_forget_bwd = gaussian(splits[4], (D, HEADS * DK), D ** -0.5, 0.125, ((1, 4),))
    w_value = gaussian(splits[5], (D, HEADS * DV), D ** -0.5, 0.125, ((1, 4),))
    decay_floor = draw_decay_floor(jax.random.fold_in(splits[17], 71), 0)
    decay_shift = draw_decay_shift(jax.random.fold_in(splits[17], 71), 0)
    head_gain = jnp.clip(1.0 + 0.18 * jax.random.normal(splits[8], (DV,), jnp.float32), 0.1, 1.9)
    w_out = gaussian(splits[9], (HEADS * DV, D), D ** -0.5, 0.125)
    moe_tokens = gaussian(splits[10], (MROWS, D), 1.0, 6.0, ((0, 8),))
    moe_gain = jnp.clip(1.0 + 0.18 * jax.random.normal(splits[11], (D,), jnp.float32), 0.1, 1.9)
    routes_keys = jax.random.split(jax.random.fold_in(splits[12], 1), MROWS // M_EP)
    routes_turns = jax.random.permutation(jax.random.fold_in(splits[12], 3), MROWS // M_EP)
    routes = jax.vmap(lambda own, number: shared_out(jax.random.fold_in(splits[12], 2), own, number, M_EP, EXPERTS, 2, CAP, 1))(routes_keys, routes_turns).reshape((MROWS, TOPK))
    route_logits = gaussian(splits[13], (MROWS, TOPK), 1.5, 6.0, ((0, 8),), jnp.float32)
    w_expert_gate = gaussian(splits[14], (EXPERTS, D, FF), D ** -0.5, 0.125, ((0, 8), (2, 4)))
    w_expert_up = gaussian(splits[15], (EXPERTS, D, FF), D ** -0.5, 0.125, ((0, 8), (2, 4)))
    w_expert_down = gaussian(splits[16], (EXPERTS, FF, D), FF ** -0.5, 0.078125, ((0, 8), (1, 4)))
    return {"mix_tokens": mix_tokens, "mix_gain": mix_gain, "w_query": w_query, "w_forget_fwd": w_forget_fwd, "w_forget_bwd": w_forget_bwd, "w_value": w_value, "decay_floor": decay_floor, "decay_shift": decay_shift, "head_gain": head_gain, "w_out": w_out, "moe_tokens": moe_tokens, "moe_gain": moe_gain, "routes": routes, "route_logits": route_logits, "w_expert_gate": w_expert_gate, "w_expert_up": w_expert_up, "w_expert_down": w_expert_down}


EPSILON = 1e-06
PRECISE = lax.Precision.HIGHEST

def rms_rows(array, norm_gain):
    floats = array.astype(jnp.float32)
    factor = lax.rsqrt(lax.optimization_barrier(jnp.mean(floats * floats, axis=-1, keepdims=True)) + EPSILON)
    return floats * factor * norm_gain

def decay_terms(pre_act, lower_bound, shifts, head_count):
    squashed = jax.nn.sigmoid(pre_act.astype(jnp.float32))
    key_rows = (1.0 - lower_bound)[None, :] * (1.0 - squashed)
    key_rows = key_rows.reshape(key_rows.shape[0], head_count, key_rows.shape[1] // head_count)
    log_decay = jnp.log1p(-key_rows) + shifts[:, :, None]
    return (key_rows, log_decay)

def sweep_blocks(queries, key_rows, values, log_decay, blk_rows):
    token_count, head_count, key_width = queries.shape
    value_width = values.shape[2]
    block_count = token_count // blk_rows
    lower_mask = jnp.tril(jnp.ones((blk_rows, blk_rows), jnp.float32))

    def to_blocks(array):
        return array.reshape(block_count, blk_rows, head_count, array.shape[2])

    def advance(carried, block):
        states, offset = carried
        block_q, block_k, block_v, block_g = block
        running = jnp.cumsum(block_g, axis=0)
        query_grown = block_q * jnp.exp(running)
        key_shrunk = block_k * jnp.exp(-running)
        scores = jnp.einsum('thd,shd->hts', query_grown, key_shrunk, precision=PRECISE) * lower_mask[None]
        result = jnp.einsum('hts,shv->thv', scores, block_v, precision=PRECISE) + jnp.einsum('thd,hdv->thv', query_grown, states, precision=PRECISE)
        block_end = running[-1]
        states = jnp.exp(block_end)[:, :, None] * states + jnp.einsum('shd,shv->hdv', block_k * jnp.exp(block_end[None] - running), block_v, precision=PRECISE)
        return ((states, offset + block_end), (result, offset[None] + running))
    starting = (jnp.zeros((head_count, key_width, value_width), jnp.float32), jnp.zeros((head_count, key_width), jnp.float32))
    blocks_in = (to_blocks(queries), to_blocks(key_rows), to_blocks(values), to_blocks(log_decay))
    (states, totals), (results, cumulative) = lax.scan(advance, starting, blocks_in)
    return (results.reshape(token_count, head_count, value_width), cumulative.reshape(token_count, head_count, key_width), totals, states)

def slot_positions(route_rows, expert_count, capacity):
    flattened = route_rows.reshape(-1)
    onehot = (flattened[:, None] == jnp.arange(expert_count, dtype=jnp.int32)[None, :]).astype(jnp.int32)
    before = jnp.cumsum(onehot, axis=0) - onehot
    slot_rank = lax.optimization_barrier(jnp.sum(before * onehot, axis=1))
    return (flattened * capacity + slot_rank).reshape(route_rows.shape).astype(jnp.int32)

def reference(mix_tokens, mix_gain, w_query, w_forget_fwd, w_forget_bwd, w_value, decay_floor, decay_shift, head_gain, w_out, moe_tokens, moe_gain, routes, route_logits, w_expert_gate, w_expert_up, w_expert_down):
    normed = rms_rows(mix_tokens, mix_gain).astype(jnp.bfloat16)

    def project(weight):
        return jnp.dot(normed, weight, preferred_element_type=jnp.float32).astype(jnp.bfloat16)
    queries = jax.nn.silu(project(w_query).astype(jnp.float32)).reshape(ROWS, HEADS, DK)
    values = project(w_value).astype(jnp.float32).reshape(ROWS, HEADS, DV)
    keys_fwd, forward_log_decay = decay_terms(project(w_forget_fwd), decay_floor, decay_shift, HEADS)
    keys_bwd, logs_bwd = decay_terms(project(w_forget_bwd), decay_floor, decay_shift, HEADS)
    out_fwd = sweep_blocks(queries, keys_fwd, values, forward_log_decay, 128)[0]
    out_bwd = sweep_blocks(jnp.flip(queries, 0), jnp.flip(keys_bwd, 0), jnp.flip(values, 0), jnp.flip(logs_bwd, 0), 128)[0]
    combined = out_fwd + jnp.flip(out_bwd, 0)
    readout = rms_rows(combined, head_gain).reshape(ROWS, HEADS * DV).astype(jnp.bfloat16)
    mixed_out = jnp.dot(readout, w_out, preferred_element_type=jnp.float32).astype(jnp.bfloat16)
    normed_moe = rms_rows(moe_tokens, moe_gain).astype(jnp.bfloat16)
    blocks = routes.reshape(N_EP, M_EP, TOPK)
    position = jax.vmap(functools.partial(slot_positions, expert_count=EXPERTS, capacity=CAP))(blocks)
    local_rows = jnp.arange(TOPK * M_EP, dtype=jnp.int32) // TOPK

    def slot_table(block_pos, source):
        filled = jnp.full((EXPERTS * CAP,), MROWS, jnp.int32)
        return filled.at[block_pos.reshape(-1)].set(source * M_EP + local_rows)
    tables = jax.vmap(slot_table)(position, jnp.arange(N_EP, dtype=jnp.int32))
    by_expert = tables.reshape(N_EP, EXPERTS, CAP).transpose(1, 0, 2).reshape(EXPERTS, N_EP * CAP)
    padded = jnp.concatenate([normed_moe, jnp.zeros((1, D), jnp.bfloat16)], axis=0)
    group_cols = FF // N_TP

    def expert_rows(expert_args):
        rows_index, gate_weight, up_weight, down_weight = expert_args
        row_data = padded[rows_index]
        gate_acts = jnp.dot(row_data, gate_weight, preferred_element_type=jnp.float32)
        up_acts = jnp.dot(row_data, up_weight, preferred_element_type=jnp.float32)
        hidden = (jax.nn.silu(gate_acts) * up_acts).astype(jnp.bfloat16)
        summed = jnp.zeros((row_data.shape[0], D), jnp.float32)
        for step_index in range(N_TP):
            partial_value = jnp.dot(hidden[:, step_index * group_cols:(step_index + 1) * group_cols], down_weight[step_index * group_cols:(step_index + 1) * group_cols], preferred_element_type=jnp.float32).astype(jnp.bfloat16)
            summed = summed + lax.optimization_barrier(partial_value).astype(jnp.float32)
        return summed.astype(jnp.bfloat16)
    results = lax.map(expert_rows, (by_expert, w_expert_gate, w_expert_up, w_expert_down))
    slot_of = position - blocks * CAP
    sources = jnp.arange(N_EP, dtype=jnp.int32)[:, None, None]
    flat_index = ((blocks * N_EP + sources) * CAP + slot_of).reshape(MROWS, TOPK)
    picked = results.reshape(EXPERTS * N_EP * CAP, D)[flat_index].astype(jnp.float32)
    weights = jax.nn.sigmoid(route_logits - jnp.flip(route_logits, 1))
    moe_out = lax.optimization_barrier(jnp.sum(picked * weights[:, :, None], axis=1)).astype(jnp.bfloat16)
    return (mixed_out, moe_out)
```

```python
import functools
import math

import jax
import jax.numpy as jnp
from jax import lax
from jax.experimental import pallas as pl
from jax.experimental.pallas import tpu as pltpu
from jax.sharding import PartitionSpec as P

DK = 128
DV = 128
EPSILON = 1e-06
BF = jnp.bfloat16
F32 = jnp.float32
CHUNKS = 2


def rms_rows(array, norm_gain):
    floats = array.astype(F32)
    factor = lax.rsqrt(jnp.mean(floats * floats, axis=-1, keepdims=True) + EPSILON)
    return floats * factor * norm_gain


def mm(a, b, ca=1, cb=0):
    return lax.dot_general(a, b, (((ca,), (cb,)), ((), ())), preferred_element_type=F32)


def sweep_kernel(blk, q_ref, f_ref, b_ref, v_ref, floor_ref, shift_ref, out_ref, grown_ref, state_ref, total_ref):
    rows = q_ref.shape[0]
    count = rows // blk
    head = pl.program_id(0)
    shift = shift_ref[...]
    lanes = lax.broadcasted_iota(jnp.int32, shift.shape, 1)
    shift = jnp.sum(jnp.where(lanes == head, shift, 0.0), axis=1, keepdims=True)
    ti = lax.broadcasted_iota(jnp.int32, (blk, blk), 0)
    si = lax.broadcasted_iota(jnp.int32, (blk, blk), 1)
    span = 1.0 - floor_ref[...]
    for way in (0, 1):
        keep = (ti >= si) if way == 0 else (ti <= si)
        ones = jnp.where(keep, 1.0, 0.0).astype(BF)
        pre_ref = f_ref if way == 0 else b_ref
        state = jnp.zeros((DK, DV), F32)
        offset = jnp.zeros((1, DK), F32)
        for step in range(count):
            block = step if way == 0 else count - 1 - step
            at = pl.ds(block * blk, blk)
            qp = q_ref[at, :].astype(F32)
            q = qp * jax.nn.sigmoid(qp)
            v = v_ref[at, :]
            k = span * (1.0 - jax.nn.sigmoid(pre_ref[at, :].astype(F32)))
            g = jnp.log1p(-k) + shift[block * blk : (block + 1) * blk]
            high = g.astype(BF)
            rest = g - high.astype(F32)
            low = rest.astype(BF)
            running = mm(ones, high) + mm(ones, low)
            end = running[blk - 1 : blk] if way == 0 else running[0:1]
            grown = q * jnp.exp(running)
            grown_bf = grown.astype(BF)
            shrunk = (k * jnp.exp(-running)).astype(BF)
            scores = jnp.where(keep, mm(grown_bf, shrunk, 1, 1), 0.0).astype(BF)
            result = mm(scores, v)
            if step > 0:
                result = result + mm(grown_bf, state.astype(BF))
            if way == 0:
                out_ref[at, :] = result
            else:
                out_ref[at, :] += result
            grown_ref[way, at, :] = (grown * jnp.exp(offset)).astype(BF)
            left = (k * jnp.exp(end - running)).astype(BF)
            update = mm(left, v, 0, 0)
            if step > 0:
                decay = jnp.exp(jnp.broadcast_to(end, (DV, DK))).T
                update = update + decay * state
            state = update
            offset = offset + end
        state_ref[way] = state.astype(BF)
        total_ref[way, 0] = offset


def sweep(q, f, b, v, floor, shift):
    rows, width = q.shape
    heads = width // DK
    blk = math.gcd(rows, 128)
    cols = pl.BlockSpec((rows, DK), lambda h: (0, h))
    return pl.pallas_call(
        functools.partial(sweep_kernel, blk),
        grid=(heads,),
        in_specs=[cols, cols, cols, cols, pl.BlockSpec((1, DK), lambda h: (0, h)), pl.BlockSpec(shift.shape, lambda h: (0, 0))],
        out_specs=[
            cols,
            pl.BlockSpec((2, rows, DK), lambda h: (0, 0, h)),
            pl.BlockSpec((2, None, DK, DV), lambda h: (0, h, 0, 0)),
            pl.BlockSpec((2, 1, 1, DK), lambda h: (0, h, 0, 0)),
        ],
        out_shape=[
            jax.ShapeDtypeStruct((rows, width), F32),
            jax.ShapeDtypeStruct((2, rows, width), BF),
            jax.ShapeDtypeStruct((2, heads, DK, DV), BF),
            jax.ShapeDtypeStruct((2, heads, 1, DK), F32),
        ],
        cost_estimate=pl.CostEstimate(flops=rows * width * 128 * 2 * 8 * 8, bytes_accessed=rows * width * 16, transcendentals=rows * width * 12),
    )(q, f, b, v, floor.reshape(1, width), shift)


def readout_kernel(out_ref, grown_ref, carry_ref, gain_ref, read_ref):
    total = out_ref[...] + mm(grown_ref[0], carry_ref[0]) + mm(grown_ref[1], carry_ref[1])
    factor = lax.rsqrt(jnp.mean(total * total, axis=1, keepdims=True) + EPSILON)
    read_ref[...] = (total * factor * gain_ref[...]).astype(BF)


def finish(out, grown, carry, gain):
    rows, width = out.shape
    cols = pl.BlockSpec((rows, DV), lambda h: (0, h))
    return pl.pallas_call(
        readout_kernel,
        grid=(width // DV,),
        in_specs=[
            cols,
            pl.BlockSpec((2, rows, DK), lambda h: (0, 0, h)),
            pl.BlockSpec((2, None, DK, DV), lambda h: (0, h, 0, 0)),
            pl.BlockSpec((1, DV), lambda h: (0, 0)),
        ],
        out_specs=cols,
        out_shape=jax.ShapeDtypeStruct((rows, width), BF),
        cost_estimate=pl.CostEstimate(flops=rows * width * 128 * 8, bytes_accessed=rows * width * 10, transcendentals=rows),
    )(out, grown, carry, gain.reshape(1, DV))


def shifted(block, axis, shift):
    count = lax.axis_size(axis)
    if shift % count == 0:
        return block
    return lax.ppermute(block, axis, [(i, (i + shift) % count) for i in range(count)])


def twin(block):
    count = lax.axis_size("tp")
    return lax.ppermute(block, "tp", [(i, i ^ 1) for i in range(count)])


def exchange_states(state, total):
    ep = lax.axis_size("ep")
    heads = state.shape[1]
    part = heads * DK // ep
    rows = state.reshape(2, ep, part, DV).transpose(1, 0, 2, 3)
    logs = total.reshape(2, ep, part).transpose(1, 0, 2)
    high = logs.astype(BF)
    low = (logs - high.astype(F32)).astype(BF)
    packed = jnp.concatenate([rows, jnp.stack([high, low], axis=3), jnp.zeros(rows.shape[:3] + (DV - 2,), BF)], axis=3)
    got = lax.all_to_all(packed, "ep", split_axis=0, concat_axis=0, tiled=True)
    logs = got[..., DV].astype(F32) + got[..., DV + 1].astype(F32)
    decay = jnp.exp(logs)[..., None]
    rows = got[..., :DV].astype(F32)
    ahead = [jnp.zeros(rows.shape[2:], F32)]
    behind = [jnp.zeros(rows.shape[2:], F32)]
    for i in range(ep - 1):
        ahead.append(decay[i, 0] * ahead[-1] + rows[i, 0])
        j = ep - 1 - i
        behind.append(decay[j, 1] * behind[-1] + rows[j, 1])
    sent = jnp.stack([jnp.stack(ahead), jnp.stack(behind[::-1])], axis=1).astype(BF)
    back = lax.all_to_all(sent, "ep", split_axis=0, concat_axis=0, tiled=True)
    return back.transpose(1, 0, 2, 3).reshape(state.shape)


def body(
    mix_tokens,
    mix_gain,
    w_query,
    w_forget_fwd,
    w_forget_bwd,
    w_value,
    decay_floor,
    decay_shift,
    head_gain,
    w_out,
    moe_tokens,
    moe_gain,
    routes,
    route_logits,
    w_expert_gate,
    w_expert_up,
    w_expert_down,
):
    tp_size = lax.axis_size("tp")
    ep_size = lax.axis_size("ep")
    token_rows, model_cols = moe_tokens.shape
    capacity = 3 * token_rows // ep_size
    part_cols = model_cols // tp_size
    normed_moe = rms_rows(moe_tokens, moe_gain).astype(BF)
    own_cols = lax.dynamic_slice_in_dim(normed_moe, lax.axis_index("tp") * part_cols, part_cols, 1)
    experts = lax.rem(jnp.arange(ep_size, dtype=jnp.int32) + lax.axis_index("ep"), ep_size)
    named = jnp.sum((routes[:, :, None] == experts).astype(F32), axis=1)
    order = jnp.arange(token_rows, dtype=jnp.int32)
    earlier = (order[:, None] > order[None, :]).astype(BF)
    before = jnp.dot(earlier, named.astype(BF), preferred_element_type=F32)
    weights = jax.nn.sigmoid(route_logits - jnp.flip(route_logits, 1))
    place = before.astype(jnp.int32)
    slots = jnp.arange(capacity, dtype=jnp.int32)
    sizes = capacity // CHUNKS
    mine = named > 0.0
    weight_of = jnp.sum(jnp.where(routes[:, :, None] == experts, weights[:, :, None], 0.0), axis=1)
    lands = (place.T[:, None, :] == slots[None, :, None]) & mine.T[:, None, :]
    picks = lands.astype(BF).reshape(ep_size * capacity, token_rows)
    outgoing = jnp.dot(picks, own_cols, preferred_element_type=F32).astype(BF)
    outgoing = outgoing.reshape(ep_size, capacity, part_cols)
    arrived = jnp.stack([shifted(outgoing[i], "ep", i) for i in range(ep_size)])
    gate_weight = w_expert_gate[0]
    up_weight = w_expert_up[0]
    down_weight = w_expert_down[0]
    chips = tp_size // 2
    place_tp = lax.axis_index("tp")
    chip, core = place_tp // 2, lax.rem(place_tp, 2)
    pieces = []
    for c in range(CHUNKS):
        own = arrived[:, c * sizes : (c + 1) * sizes].reshape(ep_size * sizes, part_cols)
        ours = [shifted(own, "tp", 2 * k) for k in range(chips)]
        theirs = [twin(a) for a in ours]
        stacked = jnp.stack(ours + theirs)
        order = []
        for t in range(tp_size):
            back = lax.rem(chip + chips - t // 2, chips)
            order.append(back + chips * jnp.where(core == t % 2, 0, 1))
        pieces.append(jnp.concatenate([lax.dynamic_index_in_dim(stacked, o, 0, False) for o in order], axis=1))

    normed = rms_rows(mix_tokens, mix_gain).astype(BF)

    def project(weight):
        return jnp.dot(normed, weight, preferred_element_type=F32).astype(BF)

    acts = [project(w) for w in (w_query, w_forget_fwd, w_forget_bwd, w_value)]
    acts, _ = lax.optimization_barrier((acts, arrived))
    out, grown, state, total = sweep(*acts, decay_floor, decay_shift)
    carry = exchange_states(state, total)
    moe = jnp.zeros((token_rows, part_cols), F32)
    for c in range(CHUNKS):
        rows = pieces[c]
        if c:
            rows, _ = lax.optimization_barrier((rows, products))
        gate_acts = jnp.dot(rows, gate_weight, preferred_element_type=F32)
        up_acts = jnp.dot(rows, up_weight, preferred_element_type=F32)
        hidden = (jax.nn.silu(gate_acts) * up_acts).astype(BF)

        def product(k, which):
            to = 2 * lax.rem(chip + k, chips) + which
            cols = lax.dynamic_slice_in_dim(down_weight, to * part_cols, part_cols, 1)
            return jnp.dot(hidden, cols, preferred_element_type=F32).astype(BF)

        ahead = list(reversed(range(chips)))
        from_twin = {k: twin(product(k, 1 - core)) for k in ahead}
        products = [product(k, core) for k in ahead]
        paired = {k: p.astype(F32) + from_twin[k].astype(F32) for k, p in zip(ahead, products)}
        summed = paired[0]
        for k in ahead[:-1]:
            summed = summed + shifted(paired[k].astype(BF), "tp", 2 * k).astype(F32)
        summed = summed.astype(BF)
        summed = summed.reshape(ep_size, sizes, part_cols)
        returned = jnp.concatenate([shifted(summed[i], "ep", -i) for i in range(ep_size)])
        here = slots[c * sizes : (c + 1) * sizes]
        lies = (place[:, :, None] == here) & mine[:, :, None]
        factor = jnp.where(lies, weight_of[:, :, None], 0.0).reshape(token_rows, ep_size * sizes)
        high = factor.astype(BF)
        low = (factor - high.astype(F32)).astype(BF)
        moe = moe + jnp.dot(high, returned, preferred_element_type=F32) + jnp.dot(low, returned, preferred_element_type=F32)
    carry, _ = lax.optimization_barrier((carry, products))
    readout = finish(out, grown, carry, head_gain)
    quarter = readout.shape[0] // tp_size
    width = readout.shape[1]
    mixed = 0.0
    for i in range(tp_size):
        to = lax.rem(place_tp + i, tp_size)
        source = lax.rem(place_tp + tp_size - i, tp_size)
        got = shifted(lax.dynamic_slice_in_dim(readout, to * quarter, quarter, 0), "tp", i)
        rows = lax.dynamic_slice_in_dim(w_out, source * width, width, 0)
        mixed = mixed + jnp.dot(got, rows, preferred_element_type=F32)
    mixed_out = mixed.astype(BF)
    return (mixed_out, moe.astype(BF))


def solution(mesh):
    return jax.shard_map(
        body,
        mesh=mesh,
        in_specs=(
            P("ep", None),
            P(),
            P(None, "tp"),
            P(None, "tp"),
            P(None, "tp"),
            P(None, "tp"),
            P("tp"),
            P("ep", "tp"),
            P(),
            P(),
            P("ep", None),
            P(),
            P("ep", None),
            P("ep", None),
            P("ep", None, "tp"),
            P("ep", None, "tp"),
            P("ep", "tp", None),
        ),
        out_specs=(P(("ep", "tp"), None), P("ep", "tp")),
        check_vma=False,
    )
```
